32 devices in a mesh: grp: 2 (over y), sp: 4 (over z), tp: 4 (over x, core).
Axes of the slice: x: 2, y: 2, z: 4, core: 2. Of those that a mesh axis runs over, the one named last changes fastest.
Arguments:
- queries: bfloat16 [2048, 1024], P(('grp', 'sp'), 'tp'), parts along dimension 0, may hold values from -7 to 10
- keys: bfloat16 [2048, 1024], P(('grp', 'sp'), 'tp'), parts along dimension 0, may hold values from -14 to 7
- values: bfloat16 [2048, 1024], P(('grp', 'sp'), 'tp'), parts along dimension 0, may hold values from -6 to 6
- resid: bfloat16 [2048, 2048], P(('grp', 'sp', 'tp')), parts along dimension 0, may hold values from -18 to 18
- out_weight: bfloat16 [1024, 2048], P('tp'), may hold values from -0.375 to 0.375
- gate_weight: bfloat16 [2048, 3072], P('sp', 'tp'), may hold values from -0.125 to 0.125
- value_weight: bfloat16 [2048, 3072], P('sp', 'tp'), may hold values from -0.125 to 0.125
- conv_gate: float32 [3, 3072], P(None, 'tp'), may hold values from -3 to 3
- conv_value: float32 [3, 3072], P(None, 'tp'), may hold values from -3 to 3
- norm_gain: float32 [2048], replicated, may hold values from 0.1 to 1.9
- down_weight: bfloat16 [3072, 2048], P('tp', 'sp'), may hold values from -0.109375 to 0.109375
Outputs:
- layer_out: bfloat16 [2048, 2048], P(('grp', 'sp', 'tp')), parts along dimension 0
The draws below stay inside these ranges and needn't reach their ends.
There are 2 independent parts, one for each index of `grp`. The reference program is written for one: setup_inputs(seed, part) draws one part's arguments, and reference() takes and returns one part's arrays. A program takes and returns all parts, laid end to end along the dimension named above; an argument that names none is the same for every part. Nothing has to cross between parts.
All inputs are finite; a program needn't handle non-finite values.
Results may differ from the reference program's by a relative error of at most 0.0058.
Values may be sent and summed in bfloat16 or wider, within the bound.
A program may use at most 128 MiB of HBM per device.

```python
import math
import jax
import jax.numpy as jnp
from jax import lax

D = 2048
HEAD_TOTAL = 16
HEAD = 64
FF = 3072
CONV = 3
TOK_DEV = 256
MIX = 1024
TOKEN_POSITIONS = 1024
KEY_BLOCK = 1024


def attention_pair(key):
    parallel_flows = jax.random.split(jax.random.fold_in(key, 11), 7)
    shape = (TOKEN_POSITIONS, HEAD_TOTAL, HEAD)
    query_noise = jnp.clip(jax.random.normal(parallel_flows[0], shape, jnp.float32), -4.5, 4.5)
    key_noise = jnp.clip(jax.random.normal(parallel_flows[1], shape, jnp.float32), -4.5, 4.5)
    fast_share = 0.5
    query_noise = query_noise * 1.4
    key_noise = key_noise * 1.4
    fast = jax.random.uniform(parallel_flows[2], (HEAD_TOTAL,), jnp.float32) < fast_share
    slow_level = -math.log(TOKEN_POSITIONS) - 2.0
    level = jnp.where(fast, -4.5, slow_level)
    block_shift = jax.random.uniform(parallel_flows[3], (TOKEN_POSITIONS // TOK_DEV, HEAD_TOTAL), jnp.float32, -0.7, 0.7)
    start_displacement = level[None, :] + jnp.repeat(block_shift, TOK_DEV, axis=0)
    surge_location = jax.random.randint(parallel_flows[4], (3, HEAD_TOTAL), 0, TOKEN_POSITIONS)
    surge_level = jax.random.uniform(parallel_flows[5], (3, HEAD_TOTAL), jnp.float32, -1.4, 0.0)
    token_position = jnp.arange(TOKEN_POSITIONS, dtype=jnp.int32)
    match_count = token_position[:, None, None] == surge_location[None, :, :]
    surge_value = jnp.max(jnp.where(match_count, surge_level[None, :, :], -100.0), axis=1)
    start_displacement = jnp.where(jnp.any(match_count, axis=1), surge_value, start_displacement)
    query_lead = 8.0 + 0.3 * jnp.clip(jax.random.normal(parallel_flows[6], (TOKEN_POSITIONS, HEAD_TOTAL), jnp.float32), -3.0, 3.0)
    query_full = query_noise.at[:, :, 0].set(query_lead)
    key_full = key_noise.at[:, :, 0].set(start_displacement)
    return (query_full.reshape(TOKEN_POSITIONS, HEAD_TOTAL * HEAD), key_full.reshape(TOKEN_POSITIONS, HEAD_TOTAL * HEAD))


def draw_queries(key, part):
    return attention_pair(key)[0].astype(jnp.bfloat16)


def draw_keys(key, part):
    return attention_pair(key)[1].astype(jnp.bfloat16)


def draw_resid(key, part):
    parallel_flows = jax.random.split(jax.random.fold_in(key, 23), 3)
    base = jnp.clip(jax.random.normal(parallel_flows[0], (TOKEN_POSITIONS, D), jnp.float32), -3.0, 3.0)
    reach = 0.6
    column_scale = jnp.exp(jax.random.uniform(parallel_flows[1], (D,), jnp.float32, -reach, reach))
    row_scale = jnp.exp(jax.random.uniform(parallel_flows[2], (TOKEN_POSITIONS,), jnp.float32, -reach, reach))
    return (base * row_scale[:, None] * column_scale[None, :]).astype(jnp.bfloat16)


def block_levels(rng, dims, cuts, low, top_value):
    gain, own = 1.0, jax.random.fold_in(rng, 6)
    for position, parts in cuts:
        steps = jnp.exp(jax.random.uniform(jax.random.fold_in(own, position), (parts,), jnp.float32, low / len(cuts), top_value / len(cuts)))
        gain = gain * jnp.repeat(steps, dims[position] // parts).reshape([-1 if axis == position else 1 for axis in range(len(dims))])
    return gain


def normal_values(key, dims, deviation, most, cuts=(), held_as=jnp.bfloat16):
    array = jax.random.normal(key, dims, jnp.float32) * deviation
    if len(cuts) > 0:
        array = block_levels(key, dims, cuts, -0.22, 0.18) * array
    return jnp.clip(array, min=-most, max=most).astype(held_as)


def setup_inputs(seed: int = 0, part: int = 0) -> dict:
    key_of = jax.random.split(jax.random.key(seed), 12)
    own_keys = jax.random.split(jax.random.fold_in(key_of[11], part), 12)
    queries = draw_queries(jax.random.fold_in(jax.random.fold_in(key_of[11], part), 71), part)
    keys = draw_keys(jax.random.fold_in(jax.random.fold_in(key_of[11], part), 71), part)
    values = normal_values(own_keys[2], (TOKEN_POSITIONS, MIX), 1.0, 6.0, ((0, 4), (1, 4)))
    resid = draw_resid(jax.random.fold_in(jax.random.fold_in(key_of[11], part), 71), part)
    out_weight = normal_values(key_of[4], (MIX, D), (MIX // 4) ** -0.5, 0.375, ((0, 4),))
    gate_weight = normal_values(key_of[5], (D, FF), D ** -0.5, 0.125, ((0, 4), (1, 4)))
    value_weight = normal_values(key_of[6], (D, FF), D ** -0.5, 0.125, ((0, 4), (1, 4)))
    conv_gate = normal_values(key_of[7], (CONV, FF), 0.5, 3.0, ((1, 4),), jnp.float32)
    conv_value = normal_values(key_of[8], (CONV, FF), 0.5, 3.0, ((1, 4),), jnp.float32)
    norm_gain = jnp.clip(1.0 + 0.18 * jax.random.normal(key_of[9], (D,), jnp.float32), 0.1, 1.9)
    down_weight = normal_values(key_of[10], (FF, D), FF ** -0.5, 0.109375, ((0, 4), (1, 4)))
    return dict(queries=queries, keys=keys, values=values, resid=resid, out_weight=out_weight, gate_weight=gate_weight, value_weight=value_weight, conv_gate=conv_gate, conv_value=conv_value, norm_gain=norm_gain, down_weight=down_weight)


epsilon = 1e-06

def block_terms(query_rows, key_rows, value_rows, query_place, key_place):
    scores = jnp.einsum('qhe,khe->hqk', query_rows.astype(jnp.float32), key_rows.astype(jnp.float32)) * HEAD ** (-0.5)
    causal = (key_place[None, :] < query_place[:, None])[None]
    stay_log = jnp.where(causal, jax.nn.log_sigmoid(-scores), 0.0)
    suffix = lax.cumsum(stay_log, axis=2, reverse=True) - stay_log
    local_weight = jnp.where(causal, jnp.exp(jax.nn.log_sigmoid(scores) + suffix), 0.0).astype(jnp.bfloat16)
    part = jnp.einsum('hqk,khe->hqe', local_weight.astype(jnp.float32), value_rows.astype(jnp.float32))
    return (lax.optimization_barrier(jnp.sum(stay_log, axis=2)), part)

def attend(queries, keys, values):
    count = TOKEN_POSITIONS // KEY_BLOCK
    query_all = queries.reshape(count, KEY_BLOCK, HEAD_TOTAL, HEAD)
    key_all = keys.reshape(count, KEY_BLOCK, HEAD_TOTAL, HEAD)
    value_all = values.reshape(count, KEY_BLOCK, HEAD_TOTAL, HEAD)
    block_ids = jnp.arange(count, dtype=jnp.int32)

    def per_query(inputs):
        query_rows, query_id = inputs
        query_place = query_id * KEY_BLOCK + jnp.arange(KEY_BLOCK, dtype=jnp.int32)

        def add_block(carry, pieces):
            key_rows, value_rows, key_id = pieces
            key_place = key_id * KEY_BLOCK + jnp.arange(KEY_BLOCK, dtype=jnp.int32)
            total, part = block_terms(query_rows, key_rows, value_rows, query_place, key_place)
            return (carry * jnp.exp(total)[:, :, None] + part, None)
        start_carry = jnp.zeros((HEAD_TOTAL, KEY_BLOCK, HEAD), jnp.float32)
        result, _ = lax.scan(add_block, start_carry, (key_all, value_all, block_ids))
        return result
    attended = lax.map(per_query, (query_all, block_ids))
    return jnp.transpose(attended, (0, 2, 1, 3)).reshape(TOKEN_POSITIONS, HEAD_TOTAL * HEAD).astype(jnp.bfloat16)

def normalize(state, norm_gain):
    values = state.astype(jnp.float32)
    scaled = values * lax.rsqrt(lax.optimization_barrier(jnp.mean(values * values, axis=-1, keepdims=True)) + epsilon)
    return (scaled * norm_gain.astype(jnp.float32)).astype(jnp.bfloat16)

def causal_conv(rows, taps):
    length = rows.shape[0]
    padded = jnp.pad(rows.astype(jnp.float32), ((taps.shape[0] - 1, 0), (0, 0)))
    total = jnp.zeros(rows.shape, jnp.float32)
    for start_displacement in range(taps.shape[0]):
        total = total + taps[start_displacement].astype(jnp.float32) * padded[start_displacement:start_displacement + length]
    return total

def reference(queries, keys, values, resid, out_weight, gate_weight, value_weight, conv_gate, conv_value, norm_gain, down_weight):
    mixed = attend(queries, keys, values)
    projected = jnp.dot(mixed, out_weight, preferred_element_type=jnp.float32)
    state = (resid.astype(jnp.float32) + projected).astype(jnp.bfloat16)
    normed = normalize(state, norm_gain)
    gate_pre = jnp.dot(normed, gate_weight, preferred_element_type=jnp.float32).astype(jnp.bfloat16)
    value_pre = jnp.dot(normed, value_weight, preferred_element_type=jnp.float32).astype(jnp.bfloat16)
    conv_gate_out = causal_conv(gate_pre, conv_gate)
    conv_value_out = causal_conv(value_pre, conv_value)
    gated = (jax.nn.silu(conv_gate_out) * conv_value_out).astype(jnp.bfloat16)
    ffn = jnp.dot(gated, down_weight, preferred_element_type=jnp.float32)
    return (state.astype(jnp.float32) + ffn).astype(jnp.bfloat16)
```

```python
import functools

import jax
import jax.numpy as jnp
from jax import lax
from jax.experimental import pallas as pl
from jax.experimental.pallas import tpu as pltpu
from jax.sharding import PartitionSpec as P

HEAD = 64


epsilon = 1e-06


def shifted(block, axis, distance):
    devices = range(lax.axis_size(axis))
    route = [(i - distance, i) for i in devices if i - distance in devices]
    return lax.ppermute(block, axis, route)


def block_terms(query_rows, key_rows, value_rows, query_place, key_place):
    scores = jnp.einsum(
        "qhe,khe->hqk", query_rows, key_rows, preferred_element_type=jnp.float32
    ) * HEAD ** (-0.5)
    causal = (key_place[None, :] < query_place[:, None])[None]
    stay_log = jnp.where(causal, jax.nn.log_sigmoid(-scores), 0.0)
    suffix = lax.cumsum(stay_log, axis=2, reverse=True) - stay_log
    local_weight = jnp.where(causal, jnp.exp(jax.nn.log_sigmoid(scores) + suffix), 0.0).astype(
        jnp.bfloat16
    )
    part = jnp.einsum("hqk,khe->hqe", local_weight, value_rows, preferred_element_type=jnp.float32)
    return (jnp.sum(stay_log, axis=2), part)


def normalize(state, norm_gain):
    values = state.astype(jnp.float32)
    scaled = values * lax.rsqrt(jnp.mean(values * values, axis=-1, keepdims=True) + epsilon)
    return (scaled * norm_gain).astype(jnp.bfloat16)


def causal_conv(rim_rows, rows, taps):
    extended = jnp.concatenate([rim_rows, rows], axis=0).astype(jnp.float32)
    length = rows.shape[0]
    total = jnp.zeros(rows.shape, jnp.float32)
    for start_displacement in range(taps.shape[0]):
        total = (
            total
            + taps[start_displacement] * extended[start_displacement : start_displacement + length]
        )
    return total


def body(
    queries,
    keys,
    values,
    resid,
    out_weight,
    gate_weight,
    value_weight,
    conv_gate,
    conv_value,
    norm_gain,
    down_weight,
):
    tok_dev = queries.shape[0]
    mix_local = queries.shape[1]
    head_count = mix_local // HEAD
    sp_count = lax.axis_size("sp")
    block = tok_dev * min(sp_count, max(1, 1024 // tok_dev))
    paired = jnp.concatenate([keys, values], axis=1)
    gathered = lax.all_gather(paired, "sp", axis=0, tiled=True)
    mine = lax.axis_index("sp")
    query_place = mine * tok_dev + jnp.arange(tok_dev, dtype=jnp.int32)
    query_rows = queries.reshape(tok_dev, head_count, HEAD)

    def add_block(index, carry):
        start = index * block
        piece = lax.dynamic_slice_in_dim(gathered, start, block, 0)
        key_rows = piece[:, :mix_local].reshape(block, head_count, HEAD)
        value_rows = piece[:, mix_local:].reshape(block, head_count, HEAD)
        key_place = start + jnp.arange(block, dtype=jnp.int32)
        total, part = block_terms(query_rows, key_rows, value_rows, query_place, key_place)
        return carry * jnp.exp(total)[:, :, None] + part

    start_carry = jnp.zeros((head_count, tok_dev, HEAD), jnp.float32)
    attended = lax.fori_loop(0, mine * tok_dev // block + 1, add_block, start_carry)
    mixed = jnp.transpose(attended, (1, 0, 2)).reshape(tok_dev, mix_local).astype(jnp.bfloat16)
    projected = lax.psum_scatter(
        jnp.dot(mixed, out_weight, preferred_element_type=jnp.float32),
        "tp",
        scatter_dimension=0,
        tiled=True,
    )
    state = (resid.astype(jnp.float32) + projected).astype(jnp.bfloat16)
    normed = lax.all_gather(normalize(state, norm_gain), "tp", axis=0, tiled=True)
    ff_local = gate_weight.shape[1]
    gate_full = jnp.dot(
        normed,
        lax.all_gather(gate_weight, "sp", axis=0, tiled=True),
        preferred_element_type=jnp.float32,
    )
    value_full = jnp.dot(
        normed,
        lax.all_gather(value_weight, "sp", axis=0, tiled=True),
        preferred_element_type=jnp.float32,
    )
    gate_pre = gate_full.astype(jnp.bfloat16)
    value_pre = value_full.astype(jnp.bfloat16)
    taps_count = conv_gate.shape[0]
    rim = jnp.concatenate(
        [gate_pre[tok_dev - taps_count + 1 :], value_pre[tok_dev - taps_count + 1 :]], axis=1
    )
    before = shifted(rim, "sp", 1)
    conv_gate_out = causal_conv(before[:, :ff_local], gate_pre, conv_gate)
    conv_value_out = causal_conv(before[:, ff_local:], value_pre, conv_value)
    gated = (jax.nn.silu(conv_gate_out) * conv_value_out).astype(jnp.bfloat16)
    partial_sum = jnp.dot(
        gated,
        lax.all_gather(down_weight, "sp", axis=1, tiled=True),
        preferred_element_type=jnp.float32,
    )
    ffn_share = lax.psum_scatter(partial_sum, "tp", scatter_dimension=0, tiled=True)
    return (state.astype(jnp.float32) + ffn_share).astype(jnp.bfloat16)


MESH = pl.DeviceIdType.MESH
LANES = 128
bf16, f32 = jnp.bfloat16, jnp.float32


def mm(a, b):
    return jnp.dot(a, b, preferred_element_type=f32)


def layer_kernel(
    n, qkv, up, down, ow, resid, gain, taps, out,
    qkv_b, up_b, down_b, mix_s, mix_r, proj, op_s, op_r, nrm, pre, gated,
    keep, c_s, c_r, x_s, x_r, z_s, z_r, state, send_sem, recv_sem,
):
    s, t, g = lax.axis_index("sp"), lax.axis_index("tp"), lax.axis_index("grp")
    core = lax.rem(t, 2)
    tc = t + 1 - 2 * core
    tx = lax.rem(t + 2, 4)
    tcx = lax.rem(tc + 2, 4)
    tok = qkv.shape[1]
    share = out.shape[0]
    width = out.shape[1]
    depth = up.shape[1]
    half, dhalf = depth // 2, down.shape[1] // 2
    ranks = list(range(1, n))
    ahead = [lax.rem(s + d, n) for d in range(n)]
    behind = [lax.rem(s + n - d, n) for d in range(n)]

    barrier = pltpu.get_barrier_semaphore()
    peers = [{"sp": ahead[d]} for d in ranks] + [{"tp": lax.rem(t + e, 4)} for e in (1, 2, 3)]
    peers = peers + [{"grp": 1 - g}]
    for peer in peers:
        pl.semaphore_signal(barrier, inc=1, device_id=peer, device_id_type=MESH)
    pl.semaphore_wait(barrier, len(peers))

    names, started = {}, []

    def slot(key):
        return names.setdefault(key, len(names))

    def remote(key, src, dst, peer):
        i = slot(key)
        return pltpu.make_async_remote_copy(
            src_ref=src, dst_ref=dst, send_sem=send_sem.at[i], recv_sem=recv_sem.at[i],
            device_id=peer, device_id_type=MESH,
        )

    def send(key, src, dst, peer):
        copy = remote(key, src, dst, peer)
        copy.start()
        started.append(copy)

    def receive(key, dst, peer):
        remote(key, dst, dst, peer).wait_recv()

    for d in ranks:
        send(("q", d), qkv.at[ahead[d]], qkv_b.at[s], {"sp": ahead[d]})
    for d in ranks:
        rows = pl.ds(pl.multiple_of(half * g, half), half)
        send(("u", d), up.at[ahead[d], rows], up_b.at[s, rows], {"sp": ahead[d]})
    qkv_b[s] = qkv[s]
    up_b[s] = up[s]
    down_b[:, 2 * dhalf :] = jnp.zeros((n, down_b.shape[1] - 2 * dhalf, down_b.shape[2]), bf16)
    down_b[s, : 2 * dhalf] = down[s]
    pre[:8] = jnp.zeros((8, pre.shape[1]), f32)
    for d in ranks:
        receive(("q", d), qkv_b.at[behind[d]], {"sp": ahead[d]})

    row = lax.broadcasted_iota(jnp.int32, (tok, tok), 0)
    col = lax.broadcasted_iota(jnp.int32, (tok, tok), 1)
    causal = col < row
    later = jnp.where(row > col, 1.0, 0.0).astype(bf16)
    lane = lax.broadcasted_iota(jnp.int32, (tok, LANES), 1)
    even = lax.rem(s, 2) == 0
    for i in range(n):
        total = jnp.zeros((tok, LANES), f32)
        carry = jnp.zeros((tok, 1), f32)
        for j in range(i, -1, -1):
            pair = qkv_b[j, :, LANES:]
            score = lax.dot_general(
                qkv_b[i, :, :LANES], pair, (((1,), (1,)), ((), ())), preferred_element_type=f32
            ) * HEAD ** (-0.5)
            soft = jnp.maximum(score, 0.0) + jnp.log(1.0 + jnp.exp(-jnp.abs(score)))
            stay = jnp.where(causal, -soft, 0.0) if i == j else -soft
            high = stay.astype(bf16)
            low = (stay - high.astype(f32)).astype(bf16)
            suffix = mm(high, later) + mm(low, later)
            weight = jnp.exp(score - soft + suffix + carry)
            if i == j:
                weight = jnp.where(causal, weight, 0.0)
            total = total + mm(weight.astype(bf16), pair)
            if j > 0:
                carry = carry + jnp.sum(stay, axis=1, keepdims=True)
        low_half = jnp.where(lane < HEAD, pltpu.roll(total, HEAD, 1), 0.0)
        high_half = jnp.where(lane < HEAD, 0.0, total)
        mix_s[i] = jnp.where(even, low_half, high_half).astype(bf16)

    for d in ranks:
        send(("m", d), mix_s.at[ahead[d]], mix_r.at[s], {"sp": ahead[d]})
    for d in ranks:
        rows = pl.ds(pl.multiple_of(dhalf * g, dhalf), dhalf)
        send(("d", d), down.at[ahead[d], rows], down_b.at[s, rows], {"sp": ahead[d]})
    mix_r[s] = mix_s[s]
    for d in ranks:
        receive(("m", d), mix_r.at[behind[d]], {"sp": ahead[d]})

    step = 512
    pairs = [mix_r[2 * p] + mix_r[2 * p + 1] for p in range(n // 2)]
    for k in range(width // step):
        cols = slice(k * step, (k + 1) * step)
        part = mm(pairs[0], ow[:LANES, cols])
        for p in range(1, n // 2):
            part = part + mm(pairs[p], ow[p * LANES : (p + 1) * LANES, cols])
        proj[:, cols] = part

    def chunk(at):
        return pl.ds(pl.multiple_of(at * share, share), share)

    for e in (2, 3, 1):
        to = lax.rem(t + e, 4)
        op_s[e - 1] = proj[chunk(to)].astype(bf16)
        send(("o", e), op_s.at[e - 1], op_r.at[e - 1], {"tp": to})
    across = {"grp": 1 - g}
    for d in ranks:
        rows = pl.ds(pl.multiple_of(half * g, half), half)
        receive(("u", d), up_b.at[behind[d], rows], {"sp": ahead[d]})
        send(("uy", d), up_b.at[behind[d], rows], up_b.at[behind[d], rows], across)
    for e in (1, 2, 3):
        receive(("o", e), op_r.at[e - 1], {"tp": lax.rem(t + e, 4)})
    summed = proj[chunk(t)] + op_r[0].astype(f32) + op_r[1].astype(f32) + op_r[2].astype(f32)
    state[...] = (resid[...].astype(f32) + summed).astype(bf16)
    values = state[...].astype(f32)
    scale = lax.rsqrt(jnp.mean(values * values, axis=-1, keepdims=True) + epsilon)

    def block(si, ti):
        return nrm.at[pl.ds(pl.multiple_of(si * tok + ti * share, share), share)]

    nrm[pl.ds(pl.multiple_of(s * tok + t * share, share), share)] = (
        values * scale * gain[...]
    ).astype(bf16)
    side, sib = {"tp": tx}, {"tp": tc}
    order = [2, 1, 3] if n == 4 else ranks
    for d in order:
        send(("nz", d), block(s, t), block(s, t), {"sp": ahead[d]})
    send(("nx", 0), block(s, t), block(s, t), side)
    send(("nc", 0), block(s, t), block(s, t), sib)
    for d in ranks:
        rows = pl.ds(pl.multiple_of(dhalf * g, dhalf), dhalf)
        receive(("d", d), down_b.at[behind[d], rows], {"sp": ahead[d]})
        send(("dy", d), down_b.at[behind[d], rows], down_b.at[behind[d], rows], across)
    receive(("nx", 0), block(s, tx), side)
    send(("ncx", 0), block(s, tx), block(s, tx), sib)
    for d in ranks:
        rows = pl.ds(pl.multiple_of(half - half * g, half), half)
        receive(("uy", d), up_b.at[behind[d], rows], across)

    def lift(si):
        at = pl.multiple_of(si * tok, tok)
        rows = pl.ds(at, tok)
        part = mm(nrm[rows, :depth], up_b[0])
        for k in range(1, n):
            part = part + mm(nrm[rows, k * depth : (k + 1) * depth], up_b[k])
        pre[pl.ds(pl.multiple_of(at + 8, 8), tok)] = part.astype(bf16).astype(f32)

    def finish(d):
        receive(("nc", d), block(behind[d], tc), sib)
        receive(("ncx", d), block(behind[d], tcx), sib)
        lift(behind[d])

    last = None
    for d in order:
        receive(("nz", d), block(behind[d], t), {"sp": ahead[d]})
        send(("nx", d), block(behind[d], t), block(behind[d], t), side)
        send(("nc", d), block(behind[d], t), block(behind[d], t), sib)
    finish(0)
    for d in order:
        receive(("nx", d), block(behind[d], tx), side)
        send(("ncx", d), block(behind[d], tx), block(behind[d], tx), sib)
        if last is not None:
            finish(last)
        last = d
    finish(last)

    count = taps.shape[0]
    for i in range(n):
        conv = jnp.zeros((tok, pre.shape[1]), f32)
        for k in range(count):
            conv = conv + taps[k : k + 1] * pre[i * tok + 9 - count + k : i * tok + 9 - count + k + tok]
        first = conv[:, :LANES]
        last_block = conv[:, 2 * LANES :]
        gated[i * tok : (i + 1) * tok, :LANES] = (
            first / (1.0 + jnp.exp(-first)) * conv[:, LANES : 2 * LANES]
        ).astype(bf16)
        tail = last_block / (1.0 + jnp.exp(-last_block)) * pltpu.roll(last_block, HEAD, 1)
        gated[i * tok : (i + 1) * tok, LANES:] = jnp.where(lane < HEAD, tail, 0.0).astype(bf16)

    for d in ranks:
        rows = pl.ds(pl.multiple_of(dhalf - dhalf * g, dhalf), dhalf)
        receive(("dy", d), down_b.at[behind[d], rows], across)

    def fold_core(d):
        receive(("rc", d), c_r.at[d], sib)
        x_s[d] = (keep[d, 1] + c_r[d, 1].astype(f32)).astype(bf16)
        send(("rx", d), x_s.at[d], x_r.at[d], side)

    previous = None
    for d in order + [0]:
        rows = pl.ds(pl.multiple_of(ahead[d] * tok, tok), tok)
        piece = gated[rows]
        for k in range(n):
            proj[:, k * depth : (k + 1) * depth] = mm(piece, down_b[k])
        keep[d, 0] = proj[chunk(t)]
        keep[d, 1] = proj[chunk(tx)]
        c_s[d, 0] = proj[chunk(tc)].astype(bf16)
        c_s[d, 1] = proj[chunk(tcx)].astype(bf16)
        send(("rc", d), c_s.at[d], c_r.at[d], sib)
        if previous is not None:
            fold_core(previous)
        previous = d
    fold_core(0)
    for d in order:
        receive(("rx", d), x_r.at[d], side)
        z_s[d - 1] = (
            keep[d, 0] + c_r[d, 0].astype(f32) + x_r[d].astype(f32)
        ).astype(bf16)
        send(("rz", d), z_s.at[d - 1], z_r.at[d - 1], {"sp": ahead[d]})
    receive(("rx", 0), x_r.at[0], side)
    result = state[...].astype(f32) + keep[0, 0] + c_r[0, 0].astype(f32) + x_r[0].astype(f32)
    for d in order:
        receive(("rz", d), z_r.at[d - 1], {"sp": ahead[d]})
        result = result + z_r[d - 1].astype(f32)
    out[...] = result.astype(bf16)
    for copy in started:
        copy.wait_send()


def fast_body(
    queries,
    keys,
    values,
    resid,
    out_weight,
    gate_weight,
    value_weight,
    conv_gate,
    conv_value,
    norm_gain,
    down_weight,
):
    n = lax.axis_size("sp")
    tok = queries.shape[0]
    share, width = resid.shape
    depth, ff_local = gate_weight.shape
    unit = ff_local // n

    def by_rank(a):
        return jnp.transpose(a.reshape(a.shape[0], n, -1), (1, 0, 2))

    q, k, v = by_rank(queries), by_rank(keys), by_rank(values)
    qkv = jnp.concatenate([q, jnp.zeros_like(q), k, v], axis=2)

    def interleave(gate, value):
        return jnp.concatenate(
            [gate[..., :LANES], value[..., :LANES], gate[..., LANES:], value[..., LANES:]], axis=-1
        )

    up = interleave(by_rank(gate_weight), by_rank(value_weight))
    mine = lax.axis_index("sp") * unit
    taps = interleave(
        lax.dynamic_slice_in_dim(conv_gate, mine, unit, 1),
        lax.dynamic_slice_in_dim(conv_value, mine, unit, 1),
    )
    down = down_weight.reshape(n, unit, down_weight.shape[1])
    vm = pl.BlockSpec(memory_space=pltpu.VMEM)
    full = n * tok
    return pl.pallas_call(
        functools.partial(layer_kernel, n),
        out_shape=jax.ShapeDtypeStruct((share, width), bf16),
        in_specs=[vm] * 7,
        out_specs=vm,
        scratch_shapes=[
            pltpu.VMEM(qkv.shape, bf16),
            pltpu.VMEM(up.shape, bf16),
            pltpu.VMEM((n, 2 * LANES, down.shape[2]), bf16),
            pltpu.VMEM((n, tok, LANES), bf16),
            pltpu.VMEM((n, tok, LANES), bf16),
            pltpu.VMEM((tok, width), f32),
            pltpu.VMEM((3, share, width), bf16),
            pltpu.VMEM((3, share, width), bf16),
            pltpu.VMEM((full, width), bf16),
            pltpu.VMEM((full + 8, 2 * unit), f32),
            pltpu.VMEM((full, 2 * LANES), bf16),
            pltpu.VMEM((n, 2, share, width), f32),
            pltpu.VMEM((n, 2, share, width), bf16),
            pltpu.VMEM((n, 2, share, width), bf16),
            pltpu.VMEM((n, share, width), bf16),
            pltpu.VMEM((n, share, width), bf16),
            pltpu.VMEM((n - 1, share, width), bf16),
            pltpu.VMEM((n - 1, share, width), bf16),
            pltpu.VMEM((share, width), bf16),
            pltpu.SemaphoreType.DMA((64,)),
            pltpu.SemaphoreType.DMA((64,)),
        ],
        compiler_params=pltpu.CompilerParams(
            collective_id=0, has_side_effects=True, vmem_limit_bytes=60 * 1024 * 1024
        ),
    )(qkv, up, down, out_weight, resid, norm_gain.reshape(1, -1), taps)


def fits(mesh, queries, gate_weight):
    sizes = dict(mesh.shape)
    n = sizes["sp"]
    mix_local = queries.shape[1] // sizes["tp"]
    unit = gate_weight.shape[1] // (sizes["tp"] * n)
    return (
        sizes["grp"] == 2
        and sizes["tp"] == 4
        and n % 2 == 0
        and mix_local == n * HEAD
        and unit == LANES + HEAD
        and queries.shape[0] // (2 * n) == 256
    )


def solution(mesh):
    placed = (
        P(("grp", "sp"), "tp"),
        P(("grp", "sp"), "tp"),
        P(("grp", "sp"), "tp"),
        P(("grp", "sp", "tp"), None),
        P("tp", None),
        P("sp", "tp"),
        P("sp", "tp"),
        P(None, "tp"),
        P(None, "tp"),
        P(),
        P("tp", "sp"),
    )

    def run(*operands):
        chosen = fast_body if fits(mesh, operands[0], operands[5]) else body
        return jax.shard_map(
            chosen,
            mesh=mesh,
            in_specs=placed,
            out_specs=P(("grp", "sp", "tp"), None),
            check_vma=False,
        )(*operands)

    return run
```

```python
import functools

import jax
import jax.numpy as jnp
from jax import lax
from jax.experimental import pallas as pl
from jax.experimental.pallas import tpu as pltpu
from jax.sharding import PartitionSpec as P

HEAD = 64


epsilon = 1e-06


def shifted(block, axis, distance):
    devices = range(lax.axis_size(axis))
    route = [(i - distance, i) for i in devices if i - distance in devices]
    return lax.ppermute(block, axis, route)


def block_terms(query_rows, key_rows, value_rows, query_place, key_place):
    scores = jnp.einsum(
        "qhe,khe->hqk", query_rows, key_rows, preferred_element_type=jnp.float32
    ) * HEAD ** (-0.5)
    causal = (key_place[None, :] < query_place[:, None])[None]
    stay_log = jnp.where(causal, jax.nn.log_sigmoid(-scores), 0.0)
    suffix = lax.cumsum(stay_log, axis=2, reverse=True) - stay_log
    local_weight = jnp.where(causal, jnp.exp(jax.nn.log_sigmoid(scores) + suffix), 0.0).astype(
        jnp.bfloat16
    )
    part = jnp.einsum("hqk,khe->hqe", local_weight, value_rows, preferred_element_type=jnp.float32)
    return (jnp.sum(stay_log, axis=2), part)


def normalize(state, norm_gain):
    values = state.astype(jnp.float32)
    scaled = values * lax.rsqrt(jnp.mean(values * values, axis=-1, keepdims=True) + epsilon)
    return (scaled * norm_gain).astype(jnp.bfloat16)


def causal_conv(rim_rows, rows, taps):
    extended = jnp.concatenate([rim_rows, rows], axis=0).astype(jnp.float32)
    length = rows.shape[0]
    total = jnp.zeros(rows.shape, jnp.float32)
    for start_displacement in range(taps.shape[0]):
        total = (
            total
            + taps[start_displacement] * extended[start_displacement : start_displacement + length]
        )
    return total


def body(
    queries,
    keys,
    values,
    resid,
    out_weight,
    gate_weight,
    value_weight,
    conv_gate,
    conv_value,
    norm_gain,
    down_weight,
):
    tok_dev = queries.shape[0]
    mix_local = queries.shape[1]
    head_count = mix_local // HEAD
    sp_count = lax.axis_size("sp")
    block = tok_dev * min(sp_count, max(1, 1024 // tok_dev))
    paired = jnp.concatenate([keys, values], axis=1)
    gathered = lax.all_gather(paired, "sp", axis=0, tiled=True)
    mine = lax.axis_index("sp")
    query_place = mine * tok_dev + jnp.arange(tok_dev, dtype=jnp.int32)
    query_rows = queries.reshape(tok_dev, head_count, HEAD)

    def add_block(index, carry):
        start = index * block
        piece = lax.dynamic_slice_in_dim(gathered, start, block, 0)
        key_rows = piece[:, :mix_local].reshape(block, head_count, HEAD)
        value_rows = piece[:, mix_local:].reshape(block, head_count, HEAD)
        key_place = start + jnp.arange(block, dtype=jnp.int32)
        total, part = block_terms(query_rows, key_rows, value_rows, query_place, key_place)
        return carry * jnp.exp(total)[:, :, None] + part

    start_carry = jnp.zeros((head_count, tok_dev, HEAD), jnp.float32)
    attended = lax.fori_loop(0, mine * tok_dev // block + 1, add_block, start_carry)
    mixed = jnp.transpose(attended, (1, 0, 2)).reshape(tok_dev, mix_local).astype(jnp.bfloat16)
    projected = lax.psum_scatter(
        jnp.dot(mixed, out_weight, preferred_element_type=jnp.float32),
        "tp",
        scatter_dimension=0,
        tiled=True,
    )
    state = (resid.astype(jnp.float32) + projected).astype(jnp.bfloat16)
    normed = lax.all_gather(normalize(state, norm_gain), "tp", axis=0, tiled=True)
    ff_local = gate_weight.shape[1]
    gate_full = jnp.dot(
        normed,
        lax.all_gather(gate_weight, "sp", axis=0, tiled=True),
        preferred_element_type=jnp.float32,
    )
    value_full = jnp.dot(
        normed,
        lax.all_gather(value_weight, "sp", axis=0, tiled=True),
        preferred_element_type=jnp.float32,
    )
    gate_pre = gate_full.astype(jnp.bfloat16)
    value_pre = value_full.astype(jnp.bfloat16)
    taps_count = conv_gate.shape[0]
    rim = jnp.concatenate(
        [gate_pre[tok_dev - taps_count + 1 :], value_pre[tok_dev - taps_count + 1 :]], axis=1
    )
    before = shifted(rim, "sp", 1)
    conv_gate_out = causal_conv(before[:, :ff_local], gate_pre, conv_gate)
    conv_value_out = causal_conv(before[:, ff_local:], value_pre, conv_value)
    gated = (jax.nn.silu(conv_gate_out) * conv_value_out).astype(jnp.bfloat16)
    partial_sum = jnp.dot(
        gated,
        lax.all_gather(down_weight, "sp", axis=1, tiled=True),
        preferred_element_type=jnp.float32,
    )
    ffn_share = lax.psum_scatter(partial_sum, "tp", scatter_dimension=0, tiled=True)
    return (state.astype(jnp.float32) + ffn_share).astype(jnp.bfloat16)


MESH = pl.DeviceIdType.MESH
LANES = 128
bf16, f32 = jnp.bfloat16, jnp.float32


def mm(a, b):
    return jnp.dot(a, b, preferred_element_type=f32)


def layer_kernel(
    n, qkv, up, down, ow, resid, gain, taps, out,
    qkv_b, up_b, down_b, mix_s, mix_r, proj, op_s, op_r, nrm, pre, gated,
    keep, c_s, c_r, x_s, x_r, z_s, z_r, state, send_sem, recv_sem,
):
    s, t, g = lax.axis_index("sp"), lax.axis_index("tp"), lax.axis_index("grp")
    core = lax.rem(t, 2)
    tc = t + 1 - 2 * core
    tx = lax.rem(t + 2, 4)
    tcx = lax.rem(tc + 2, 4)
    tok = qkv.shape[1]
    share = out.shape[0]
    width = out.shape[1]
    depth = up.shape[1]
    half, dhalf = depth // 2, down.shape[1] // 2
    ranks = list(range(1, n))
    ahead = [lax.rem(s + d, n) for d in range(n)]
    behind = [lax.rem(s + n - d, n) for d in range(n)]

    barrier = pltpu.get_barrier_semaphore()
    peers = [{"sp": ahead[d]} for d in ranks] + [{"tp": lax.rem(t + e, 4)} for e in (1, 2, 3)]
    peers = peers + [{"grp": 1 - g}]
    for peer in peers:
        pl.semaphore_signal(barrier, inc=1, device_id=peer, device_id_type=MESH)
    pl.semaphore_wait(barrier, len(peers))

    names, started = {}, []

    def slot(key):
        return names.setdefault(key, len(names))

    def remote(key, src, dst, peer):
        i = slot(key)
        return pltpu.make_async_remote_copy(
            src_ref=src, dst_ref=dst, send_sem=send_sem.at[i], recv_sem=recv_sem.at[i],
            device_id=peer, device_id_type=MESH,
        )

    def send(key, src, dst, peer):
        copy = remote(key, src, dst, peer)
        copy.start()
        started.append(copy)

    def receive(key, dst, peer):
        remote(key, dst, dst, peer).wait_recv()

    for d in ranks:
        send(("q", d), qkv.at[ahead[d]], qkv_b.at[s], {"sp": ahead[d]})

    def send_up(d):
        rows = pl.ds(pl.multiple_of(half * g, half), half)
        send(("u", d), up.at[ahead[d], rows], up_b.at[s, rows], {"sp": ahead[d]})

    send_up(1)
    qkv_b[s] = qkv[s]
    up_b[s] = up[s]
    down_b[:, 2 * dhalf :] = jnp.zeros((n, down_b.shape[1] - 2 * dhalf, down_b.shape[2]), bf16)
    down_b[s, : 2 * dhalf] = down[s]
    pre[:8] = jnp.zeros((8, pre.shape[1]), f32)
    for d in ranks:
        receive(("q", d), qkv_b.at[behind[d]], {"sp": ahead[d]})

    row = lax.broadcasted_iota(jnp.int32, (tok, tok), 0)
    col = lax.broadcasted_iota(jnp.int32, (tok, tok), 1)
    causal = col < row
    later = jnp.where(row > col, 1.0, 0.0).astype(bf16)
    lane = lax.broadcasted_iota(jnp.int32, (tok, LANES), 1)
    even = lax.rem(s, 2) == 0
    for i in range(n):
        total = jnp.zeros((tok, LANES), f32)
        carry = jnp.zeros((tok, 1), f32)
        for j in range(i, -1, -1):
            pair = qkv_b[j, :, LANES:]
            score = lax.dot_general(
                qkv_b[i, :, :LANES], pair, (((1,), (1,)), ((), ())), preferred_element_type=f32
            ) * HEAD ** (-0.5)
            soft = jnp.maximum(score, 0.0) + jnp.log(1.0 + jnp.exp(-jnp.abs(score)))
            stay = jnp.where(causal, -soft, 0.0) if i == j else -soft
            high = stay.astype(bf16)
            low = (stay - high.astype(f32)).astype(bf16)
            suffix = mm(high, later) + mm(low, later)
            weight = jnp.exp(score - soft + suffix + carry)
            if i == j:
                weight = jnp.where(causal, weight, 0.0)
            total = total + mm(weight.astype(bf16), pair)
            if j > 0:
                carry = carry + jnp.sum(stay, axis=1, keepdims=True)
        low_half = jnp.where(lane < HEAD, pltpu.roll(total, HEAD, 1), 0.0)
        high_half = jnp.where(lane < HEAD, 0.0, total)
        mix_s[i] = jnp.where(even, low_half, high_half).astype(bf16)

    for d in ranks:
        send(("m", d), mix_s.at[ahead[d]], mix_r.at[s], {"sp": ahead[d]})
    for d in ranks[1:]:
        send_up(d)
    mix_r[s] = mix_s[s]
    for d in ranks:
        receive(("m", d), mix_r.at[behind[d]], {"sp": ahead[d]})

    step = 512
    pairs = [mix_r[2 * p] + mix_r[2 * p + 1] for p in range(n // 2)]
    for k in range(width // step):
        cols = slice(k * step, (k + 1) * step)
        part = mm(pairs[0], ow[:LANES, cols])
        for p in range(1, n // 2):
            part = part + mm(pairs[p], ow[p * LANES : (p + 1) * LANES, cols])
        proj[:, cols] = part

    def chunk(at):
        return pl.ds(pl.multiple_of(at * share, share), share)

    for e in (2, 3, 1):
        to = lax.rem(t + e, 4)
        op_s[e - 1] = proj[chunk(to)].astype(bf16)
        send(("o", e), op_s.at[e - 1], op_r.at[e - 1], {"tp": to})
    across = {"grp": 1 - g}
    for e in (1, 2, 3):
        receive(("o", e), op_r.at[e - 1], {"tp": lax.rem(t + e, 4)})
    summed = proj[chunk(t)] + op_r[0].astype(f32) + op_r[1].astype(f32) + op_r[2].astype(f32)
    state[...] = (resid[...].astype(f32) + summed).astype(bf16)
    values = state[...].astype(f32)
    scale = lax.rsqrt(jnp.mean(values * values, axis=-1, keepdims=True) + epsilon)

    def block(si, ti):
        return nrm.at[pl.ds(pl.multiple_of(si * tok + ti * share, share), share)]

    nrm[pl.ds(pl.multiple_of(s * tok + t * share, share), share)] = (
        values * scale * gain[...]
    ).astype(bf16)
    side, sib = {"tp": tx}, {"tp": tc}
    order = [2, 1, 3] if n == 4 else ranks
    for d in order:
        send(("nz", d), block(s, t), block(s, t), {"sp": ahead[d]})
    send(("nx", 0), block(s, t), block(s, t), side)
    send(("nc", 0), block(s, t), block(s, t), sib)
    for d in ranks:
        rows = pl.ds(pl.multiple_of(dhalf * g, dhalf), dhalf)
        send(("d", d), down.at[ahead[d], rows], down_b.at[s, rows], {"sp": ahead[d]})
    for d in ranks:
        rows = pl.ds(pl.multiple_of(half * g, half), half)
        receive(("u", d), up_b.at[behind[d], rows], {"sp": ahead[d]})
        send(("uy", d), up_b.at[behind[d], rows], up_b.at[behind[d], rows], across)
    receive(("nx", 0), block(s, tx), side)
    send(("ncx", 0), block(s, tx), block(s, tx), sib)

    def lift(si):
        at = pl.multiple_of(si * tok, tok)
        rows = pl.ds(at, tok)
        part = mm(nrm[rows, :depth], up_b[0])
        for k in range(1, n):
            part = part + mm(nrm[rows, k * depth : (k + 1) * depth], up_b[k])
        pre[pl.ds(pl.multiple_of(at + 8, 8), tok)] = part.astype(bf16).astype(f32)

    def finish(d):
        receive(("nc", d), block(behind[d], tc), sib)
        receive(("ncx", d), block(behind[d], tcx), sib)
        lift(behind[d])

    last = None
    for d in order:
        receive(("nz", d), block(behind[d], t), {"sp": ahead[d]})
        send(("nx", d), block(behind[d], t), block(behind[d], t), side)
        send(("nc", d), block(behind[d], t), block(behind[d], t), sib)
    for d in ranks:
        rows = pl.ds(pl.multiple_of(half - half * g, half), half)
        receive(("uy", d), up_b.at[behind[d], rows], across)
    finish(0)
    for d in order:
        receive(("nx", d), block(behind[d], tx), side)
        send(("ncx", d), block(behind[d], tx), block(behind[d], tx), sib)
        if last is not None:
            finish(last)
        last = d
    for d in ranks:
        rows = pl.ds(pl.multiple_of(dhalf * g, dhalf), dhalf)
        receive(("d", d), down_b.at[behind[d], rows], {"sp": ahead[d]})
        send(("dy", d), down_b.at[behind[d], rows], down_b.at[behind[d], rows], across)
    finish(last)

    count = taps.shape[0]
    for i in range(n):
        conv = jnp.zeros((tok, pre.shape[1]), f32)
        for k in range(count):
            conv = conv + taps[k : k + 1] * pre[i * tok + 9 - count + k : i * tok + 9 - count + k + tok]
        first = conv[:, :LANES]
        last_block = conv[:, 2 * LANES :]
        gated[i * tok : (i + 1) * tok, :LANES] = (
            first / (1.0 + jnp.exp(-first)) * conv[:, LANES : 2 * LANES]
        ).astype(bf16)
        tail = last_block / (1.0 + jnp.exp(-last_block)) * pltpu.roll(last_block, HEAD, 1)
        gated[i * tok : (i + 1) * tok, LANES:] = jnp.where(lane < HEAD, tail, 0.0).astype(bf16)

    for d in ranks:
        rows = pl.ds(pl.multiple_of(dhalf - dhalf * g, dhalf), dhalf)
        receive(("dy", d), down_b.at[behind[d], rows], across)

    def fold_core(d):
        receive(("rc", d), c_r.at[d], sib)
        x_s[d] = (keep[d, 1] + c_r[d, 1].astype(f32)).astype(bf16)
        send(("rx", d), x_s.at[d], x_r.at[d], side)

    previous = None
    for d in order + [0]:
        rows = pl.ds(pl.multiple_of(ahead[d] * tok, tok), tok)
        piece = gated[rows]
        for k in range(n):
            proj[:, k * depth : (k + 1) * depth] = mm(piece, down_b[k])
        keep[d, 0] = proj[chunk(t)]
        keep[d, 1] = proj[chunk(tx)]
        c_s[d, 0] = proj[chunk(tc)].astype(bf16)
        c_s[d, 1] = proj[chunk(tcx)].astype(bf16)
        send(("rc", d), c_s.at[d], c_r.at[d], sib)
        if previous is not None:
            fold_core(previous)
        previous = d
    fold_core(0)
    for d in order:
        receive(("rx", d), x_r.at[d], side)
        z_s[d - 1] = (
            keep[d, 0] + c_r[d, 0].astype(f32) + x_r[d].astype(f32)
        ).astype(bf16)
        send(("rz", d), z_s.at[d - 1], z_r.at[d - 1], {"sp": ahead[d]})
    receive(("rx", 0), x_r.at[0], side)
    result = state[...].astype(f32) + keep[0, 0] + c_r[0, 0].astype(f32) + x_r[0].astype(f32)
    for d in order:
        receive(("rz", d), z_r.at[d - 1], {"sp": ahead[d]})
        result = result + z_r[d - 1].astype(f32)
    out[...] = result.astype(bf16)
    for copy in started:
        copy.wait_send()


def fast_body(
    queries,
    keys,
    values,
    resid,
    out_weight,
    gate_weight,
    value_weight,
    conv_gate,
    conv_value,
    norm_gain,
    down_weight,
):
    n = lax.axis_size("sp")
    tok = queries.shape[0]
    share, width = resid.shape
    depth, ff_local = gate_weight.shape
    unit = ff_local // n

    def by_rank(a):
        return jnp.transpose(a.reshape(a.shape[0], n, -1), (1, 0, 2))

    q, k, v = by_rank(queries), by_rank(keys), by_rank(values)
    qkv = jnp.concatenate([q, jnp.zeros_like(q), k, v], axis=2)

    def interleave(gate, value):
        return jnp.concatenate(
            [gate[..., :LANES], value[..., :LANES], gate[..., LANES:], value[..., LANES:]], axis=-1
        )

    up = interleave(by_rank(gate_weight), by_rank(value_weight))
    mine = lax.axis_index("sp") * unit
    taps = interleave(
        lax.dynamic_slice_in_dim(conv_gate, mine, unit, 1),
        lax.dynamic_slice_in_dim(conv_value, mine, unit, 1),
    )
    down = down_weight.reshape(n, unit, down_weight.shape[1])
    vm = pl.BlockSpec(memory_space=pltpu.VMEM)
    full = n * tok
    return pl.pallas_call(
        functools.partial(layer_kernel, n),
        out_shape=jax.ShapeDtypeStruct((share, width), bf16),
        in_specs=[vm] * 7,
        out_specs=vm,
        scratch_shapes=[
            pltpu.VMEM(qkv.shape, bf16),
            pltpu.VMEM(up.shape, bf16),
            pltpu.VMEM((n, 2 * LANES, down.shape[2]), bf16),
            pltpu.VMEM((n, tok, LANES), bf16),
            pltpu.VMEM((n, tok, LANES), bf16),
            pltpu.VMEM((tok, width), f32),
            pltpu.VMEM((3, share, width), bf16),
            pltpu.VMEM((3, share, width), bf16),
            pltpu.VMEM((full, width), bf16),
            pltpu.VMEM((full + 8, 2 * unit), f32),
            pltpu.VMEM((full, 2 * LANES), bf16),
            pltpu.VMEM((n, 2, share, width), f32),
            pltpu.VMEM((n, 2, share, width), bf16),
            pltpu.VMEM((n, 2, share, width), bf16),
            pltpu.VMEM((n, share, width), bf16),
            pltpu.VMEM((n, share, width), bf16),
            pltpu.VMEM((n - 1, share, width), bf16),
            pltpu.VMEM((n - 1, share, width), bf16),
            pltpu.VMEM((share, width), bf16),
            pltpu.SemaphoreType.DMA((64,)),
            pltpu.SemaphoreType.DMA((64,)),
        ],
        compiler_params=pltpu.CompilerParams(
            collective_id=0, has_side_effects=True, vmem_limit_bytes=60 * 1024 * 1024
        ),
    )(qkv, up, down, out_weight, resid, norm_gain.reshape(1, -1), taps)


def fits(mesh, queries, gate_weight):
    sizes = dict(mesh.shape)
    n = sizes["sp"]
    mix_local = queries.shape[1] // sizes["tp"]
    unit = gate_weight.shape[1] // (sizes["tp"] * n)
    return (
        sizes["grp"] == 2
        and sizes["tp"] == 4
        and n % 2 == 0
        and mix_local == n * HEAD
        and unit == LANES + HEAD
        and queries.shape[0] // (2 * n) == 256
    )


def solution(mesh):
    placed = (
        P(("grp", "sp"), "tp"),
        P(("grp", "sp"), "tp"),
        P(("grp", "sp"), "tp"),
        P(("grp", "sp", "tp"), None),
        P("tp", None),
        P("sp", "tp"),
        P("sp", "tp"),
        P(None, "tp"),
        P(None, "tp"),
        P(),
        P("tp", "sp"),
    )

    def run(*operands):
        chosen = fast_body if fits(mesh, operands[0], operands[5]) else body
        return jax.shard_map(
            chosen,
            mesh=mesh,
            in_specs=placed,
            out_specs=P(("grp", "sp", "tp"), None),
            check_vma=False,
        )(*operands)

    return run
```
